32 devices in a mesh: kv: 8 (over z, x), tp: 4 (over y, core).
Axes of the slice: x: 2, y: 2, z: 4, core: 2. Of those that a mesh axis runs over, the one named last changes fastest.
Arguments:
- hidden: bfloat16 [128, 4, 2048], P(None, None, 'kv'), may hold values from -18 to 18
- norm_gain: float32 [2048], replicated, may hold values from 0.1 to 1.9
- w_query: bfloat16 [2048, 1024], P(None, 'tp'), may hold values from -0.125 to 0.125
- w_forget: bfloat16 [2048, 1024], P(None, 'tp'), may hold values from -0.125 to 0.125
- w_input: bfloat16 [2048, 1024], P(None, 'tp'), may hold values from -0.125 to 0.125
- w_outgate: bfloat16 [2048, 1024], P(None, 'tp'), may hold values from -0.125 to 0.125
- w_out: bfloat16 [1024, 2048], replicated, may hold values from -0.1875 to 0.1875
- floor: float32 [1024], P('tp'), may hold values from 0 to 0.95
- head_gain: float32 [128], replicated, may hold values from 0.1 to 1.9
- base_state: float32 [128, 8, 128, 128], P('kv', 'tp'), may hold values from -4 to 4
- prev_forget: bfloat16 [128, 4, 1024], P('kv', None, 'tp'), may hold values from -6 to 6
- prev_input: bfloat16 [128, 4, 1024], P('kv', None, 'tp'), may hold values from -6 to 6
- accepted: int32 [128], P('kv'), may hold values from 0 to 4
Outputs:
- mixed: bfloat16 [128, 4, 2048], P(None, None, 'kv')
- taken_state: float32 [128, 8, 128, 128], P('kv', 'tp')
The draws below stay inside these ranges and needn't reach their ends.
All inputs are finite; a program needn't handle non-finite values.
Results may differ from the reference program's by a relative error of at most 0.014.
Values may be sent and summed in bfloat16 or wider, within the bound.
A program may use at most 64 MiB of HBM per device.

```python
import jax
import jax.numpy as jnp
from jax import lax

D = 2048
HEADS = 8
HEAD_DIM = 128
PROPS = 4
SEQ_DEV = 16
WIDTH = 1024
SEQS = 128
N_KV = 8


def draw_hidden(key, part):
    columns = jnp.arange(D, dtype=jnp.float32) / D
    base = jnp.clip(jax.random.normal(key, (SEQ_DEV * N_KV, PROPS, D), jnp.float32), -6.0, 6.0)
    return (base * 3.0 ** columns).astype(jnp.bfloat16)


def touch_ends(entries, stream_key, smallest, top_value):
    longest = entries.shape.index(max(entries.shape))
    spots = []
    for shift in (0, 1):
        where = [jax.random.randint(jax.random.fold_in(stream_key, axis), (), 0, length) for axis, length in enumerate(entries.shape)]
        where[longest] = (where[longest] + shift) % entries.shape[longest]
        spots.append(tuple(where))
    return entries.at[spots[0]].set(smallest).at[spots[1]].set(top_value)


def levels(stream_key, shape, pieces, least, high):
    def one(dim, parts):
        steps = jax.random.uniform(jax.random.fold_in(jax.random.fold_in(stream_key, 6), dim), (parts,), jnp.float32, least / len(pieces), high / len(pieces))
        return jnp.repeat(jnp.exp(steps), shape[dim] // parts).reshape((-1,) + (1,) * (len(shape) - dim - 1))

    loudness = one(*pieces[0])
    for cut in pieces[1:]:
        loudness = loudness * one(*cut)
    return loudness


def centred(key, extent, width, reach, cuts=(), held_as=jnp.bfloat16):
    loudness = levels(key, extent, cuts, -0.22, 0.18) if cuts else 1.0
    values = jax.random.normal(key, extent, jnp.float32) * width * loudness
    return jnp.minimum(jnp.maximum(values, -reach), reach).astype(held_as)


def setup_inputs(seed: int = 0) -> dict:
    splits = jax.random.split(jax.random.key(seed), 14)
    hidden = draw_hidden(jax.random.fold_in(splits[13], 71), 0)
    norm_gain = jnp.clip(1.0 + 0.18 * jax.random.normal(splits[1], (D,), jnp.float32), 0.1, 1.9)
    w_query = centred(splits[2], (D, WIDTH), D ** -0.5, 0.125, ((1, 4),))
    w_forget = centred(splits[3], (D, WIDTH), D ** -0.5, 0.125, ((1, 4),))
    w_input = centred(splits[4], (D, WIDTH), D ** -0.5, 0.125, ((1, 4),))
    w_outgate = centred(splits[5], (D, WIDTH), D ** -0.5, 0.125, ((1, 4),))
    w_out = centred(splits[6], (WIDTH, D), WIDTH ** -0.5, 0.1875)
    floor = jnp.clip(0.95 * jax.random.uniform(splits[7], (WIDTH,), jnp.float32) ** levels(splits[7], (WIDTH,), ((0, 4),), -0.2, 0.2), 0.0, 0.95)
    head_gain = jnp.clip(1.0 + 0.18 * jax.random.normal(splits[8], (HEAD_DIM,), jnp.float32), 0.1, 1.9)
    base_state = centred(splits[9], (SEQS, HEADS, HEAD_DIM, HEAD_DIM), 0.3, 4.0, ((0, 8), (1, 4)), jnp.float32)
    prev_forget = centred(splits[10], (SEQS, PROPS, WIDTH), 1.5, 6.0, ((0, 8), (2, 4)))
    prev_input = centred(splits[11], (SEQS, PROPS, WIDTH), 1.0, 6.0, ((0, 8), (2, 4)))
    accepted = touch_ends(jax.random.randint(splits[12], (SEQS,), 0, PROPS + 1), jax.random.fold_in(splits[12], 1), 0, PROPS).astype(jnp.int32)
    return {"hidden": hidden, "norm_gain": norm_gain, "w_query": w_query, "w_forget": w_forget, "w_input": w_input, "w_outgate": w_outgate, "w_out": w_out, "floor": floor, "head_gain": head_gain, "base_state": base_state, "prev_forget": prev_forget, "prev_input": prev_input, "accepted": accepted}


def reference(hidden, norm_gain, w_query, w_forget, w_input, w_outgate, w_out, floor, head_gain, base_state, prev_forget, prev_input, accepted):
    values_in = hidden.astype(jnp.float32)
    squares = lax.optimization_barrier(jnp.sum(values_in * values_in, axis=2))
    normed = (values_in * lax.rsqrt(squares / D + 1e-06)[..., None] * norm_gain).astype(jnp.bfloat16)
    query_pre = jnp.dot(normed, w_query, preferred_element_type=jnp.float32).astype(jnp.bfloat16)
    forget_pre = jnp.dot(normed, w_forget, preferred_element_type=jnp.float32).astype(jnp.bfloat16)
    input_pre = jnp.dot(normed, w_input, preferred_element_type=jnp.float32).astype(jnp.bfloat16)
    gate_pre = jnp.dot(normed, w_outgate, preferred_element_type=jnp.float32).astype(jnp.bfloat16)
    seqs = hidden.shape[0]
    shape = (seqs, PROPS, HEADS, HEAD_DIM)
    query = jax.nn.silu(query_pre.astype(jnp.float32)).reshape(shape)
    forget = (floor + (1.0 - floor) * jax.nn.sigmoid(forget_pre.astype(jnp.float32))).reshape(shape)
    value = input_pre.astype(jnp.float32).reshape(shape)
    prev_f = (floor + (1.0 - floor) * jax.nn.sigmoid(prev_forget.astype(jnp.float32))).reshape(shape)
    prev_v = prev_input.astype(jnp.float32).reshape(shape)
    state = base_state
    for step in range(PROPS):
        live = (step < accepted)[:, None, None, None]
        moved = prev_f[:, step][..., None] * state + (1.0 - prev_f[:, step])[..., None] * prev_v[:, step][:, :, None, :]
        state = jnp.where(live, moved, state)
    taken_state = state
    outputs = []
    for step in range(PROPS):
        state = forget[:, step][..., None] * state + (1.0 - forget[:, step])[..., None] * value[:, step][:, :, None, :]
        outputs.append(jnp.einsum('bhk,bhkv->bhv', query[:, step], state, precision=lax.Precision.HIGHEST))
    result = jnp.stack(outputs, axis=1)
    scaled = result * lax.rsqrt(lax.optimization_barrier(jnp.mean(result * result, axis=-1, keepdims=True)) + 1e-05) * head_gain
    gated = scaled * jax.nn.silu(gate_pre.astype(jnp.float32)).reshape(shape)
    mixed_heads = gated.reshape(seqs, PROPS, HEADS * HEAD_DIM).astype(jnp.bfloat16)
    mixed = jnp.dot(mixed_heads, w_out, preferred_element_type=jnp.float32).astype(jnp.bfloat16)
    return (mixed, taken_state)
```

```python
import functools

import jax
import jax.numpy as jnp
from jax import lax
from jax.experimental import pallas as pl
from jax.experimental.pallas import tpu as pltpu
from jax.sharding import PartitionSpec as P

D = 2048
HEAD_DIM = 128
PROPS = 4


def shards(
    hidden,
    norm_gain,
    w_query,
    w_forget,
    w_input,
    w_outgate,
    w_out,
    floor,
    head_gain,
    base_state,
    prev_forget,
    prev_input,
    accepted,
):
    arrived = lax.all_to_all(hidden, "kv", split_axis=0, concat_axis=2, tiled=True)
    whole_vals = arrived.astype(jnp.float32)
    row_sums = jnp.sum(whole_vals * whole_vals, axis=2)
    normed = (whole_vals * lax.rsqrt(row_sums / D + 1e-06)[..., None] * norm_gain).astype(
        jnp.bfloat16
    )
    query_pre = jnp.dot(normed, w_query, preferred_element_type=jnp.float32).astype(jnp.bfloat16)
    forget_pre = jnp.dot(normed, w_forget, preferred_element_type=jnp.float32).astype(jnp.bfloat16)
    input_pre = jnp.dot(normed, w_input, preferred_element_type=jnp.float32).astype(jnp.bfloat16)
    gate_pre = jnp.dot(normed, w_outgate, preferred_element_type=jnp.float32).astype(jnp.bfloat16)
    seq_local = normed.shape[0]
    head_local = w_query.shape[1] // HEAD_DIM
    shape = (seq_local, PROPS, head_local, HEAD_DIM)
    query = jax.nn.silu(query_pre.astype(jnp.float32)).reshape(shape)
    forget = (floor + (1.0 - floor) * jax.nn.sigmoid(forget_pre.astype(jnp.float32))).reshape(shape)
    value = input_pre.astype(jnp.float32).reshape(shape)
    prev_f = (floor + (1.0 - floor) * jax.nn.sigmoid(prev_forget.astype(jnp.float32))).reshape(
        shape
    )
    prev_v = prev_input.astype(jnp.float32).reshape(shape)
    state = base_state
    for step in range(PROPS):
        live = (step < accepted)[:, None, None, None]
        moved = (
            prev_f[:, step][..., None] * state
            + (1.0 - prev_f[:, step])[..., None] * prev_v[:, step][:, :, None, :]
        )
        state = jnp.where(live, moved, state)
    taken_state = state
    outputs = []
    for step in range(PROPS):
        state = (
            forget[:, step][..., None] * state
            + (1.0 - forget[:, step])[..., None] * value[:, step][:, :, None, :]
        )
        outputs.append(
            jnp.einsum("bhk,bhkv->bhv", query[:, step], state, precision=lax.Precision.HIGHEST)
        )
    result = jnp.stack(outputs, axis=1)
    scaled = (
        result * lax.rsqrt(jnp.mean(result * result, axis=-1, keepdims=True) + 1e-05) * head_gain
    )
    gated = scaled * jax.nn.silu(gate_pre.astype(jnp.float32)).reshape(shape)
    mixed_heads = gated.reshape(seq_local, PROPS, head_local * HEAD_DIM).astype(jnp.bfloat16)
    own_rows = mixed_heads.shape[2]
    w_rows = lax.dynamic_slice_in_dim(w_out, lax.axis_index("tp") * own_rows, own_rows, 0)
    partial_value = jnp.dot(mixed_heads, w_rows, preferred_element_type=jnp.float32)
    finished = lax.psum(partial_value, "tp").astype(jnp.bfloat16)
    mixed = lax.all_to_all(finished, "kv", split_axis=2, concat_axis=0, tiled=True)
    return (mixed, taken_state)


def fused_kernel(
    n_kv,
    n_tp,
    accepted,
    hidden,
    gain,
    w_query,
    w_forget,
    w_input,
    w_outgate,
    w_out,
    floor,
    head_gain,
    base_state,
    prev_forget,
    prev_input,
    out,
    taken,
    hid,
    arrived,
    gain_v,
    w_all,
    w_o,
    floor_v,
    head_gain_v,
    state,
    state16,
    prev_f_v,
    prev_i_v,
    acc,
    heads_all,
    blocks,
    landed,
    local_sem,
    wo_sem,
    taken_sem,
    in_send,
    in_recv,
    fwd_send,
    fwd_recv,
    tp_send,
    tp_recv,
    out_send,
    out_recv,
    ofwd_send,
    ofwd_recv,
):
    f32, bf16 = jnp.float32, jnp.bfloat16
    seqs, props = hid.shape[0] // n_kv, hid.shape[1]
    cols = hid.shape[2]
    rows = seqs * props
    half_seq = seqs // 2
    width = w_query.shape[1]
    head_local = width // HEAD_DIM
    half_cols = cols // 2
    depth = n_kv * cols
    kv, tp = lax.axis_index("kv"), lax.axis_index("tp")
    core = lax.rem(tp, 2)
    peer = tp + 1 - 2 * core

    locals_ = [
        pltpu.make_async_copy(hidden, hid, local_sem.at[0]),
        pltpu.make_async_copy(prev_forget, prev_f_v, local_sem.at[1]),
        pltpu.make_async_copy(prev_input, prev_i_v, local_sem.at[2]),
        pltpu.make_async_copy(floor, floor_v, local_sem.at[3]),
        pltpu.make_async_copy(base_state, state, local_sem.at[4]),
        pltpu.make_async_copy(gain, gain_v, local_sem.at[5]),
        pltpu.make_async_copy(head_gain, head_gain_v, local_sem.at[6]),
    ]
    for place, weight in enumerate((w_query, w_forget, w_input, w_outgate)):
        locals_.append(
            pltpu.make_async_copy(
                weight, w_all.at[:, pl.ds(place * width, width)], local_sem.at[7 + place]
            )
        )
    w_o_copies = [
        pltpu.make_async_copy(
            w_out.at[:, pl.ds(pl.multiple_of(k * cols + core * half_cols, half_cols), half_cols)],
            w_o.at[:, pl.ds(k * half_cols, half_cols)],
            wo_sem.at[k],
        )
        for k in range(n_kv)
    ]
    barrier = pltpu.get_barrier_semaphore()
    for step in range(1, n_kv):
        pl.semaphore_signal(
            barrier,
            inc=1,
            device_id={"kv": lax.rem(kv + step, n_kv)},
            device_id_type=pl.DeviceIdType.MESH,
        )
    for step in range(1, n_tp):
        pl.semaphore_signal(
            barrier,
            inc=1,
            device_id={"tp": lax.rem(tp + step, n_tp)},
            device_id_type=pl.DeviceIdType.MESH,
        )
    for copy in locals_:
        copy.start()
    for copy in w_o_copies:
        copy.start()
    locals_[0].wait()
    pl.semaphore_wait(barrier, n_kv + n_tp - 2)

    def remote(source, target, send, recv, device):
        return pltpu.make_async_remote_copy(
            src_ref=source,
            dst_ref=target,
            send_sem=send,
            recv_sem=recv,
            device_id=device,
            device_id_type=pl.DeviceIdType.MESH,
        )

    order = sorted(range(1, n_kv), key=lambda step: -min(step, n_kv - step))
    mine = pl.ds(core * half_seq, half_seq)
    in_copies = {}
    for step in order:
        to = lax.rem(kv + step, n_kv)
        in_copies[step] = remote(
            hid.at[pl.ds(to * seqs + core * half_seq, half_seq)],
            arrived.at[kv, mine],
            in_send.at[step],
            in_recv.at[step],
            {"kv": to},
        )
        in_copies[step].start()

    for copy in locals_[1:5]:
        copy.wait()
    low = floor_v[...]
    row = lax.broadcasted_iota(jnp.int32, (rows, width), 0)
    at = lax.rem(row, props)
    seq_of = lax.div(row, props)
    taken_count = jnp.zeros((rows, width), jnp.int32)
    for s in range(seqs):
        taken_count = jnp.where(seq_of == s, accepted[s], taken_count)
    live = at < taken_count
    prev_f = low + (1.0 - low) * jax.nn.sigmoid(
        prev_f_v[...].astype(f32).reshape(rows, width)
    )
    prev_v = prev_i_v[...].astype(f32).reshape(rows, width)
    decay = jnp.where(live, prev_f, 1.0)
    enter = jnp.where(live, 1.0 - prev_f, 0.0)
    later = jnp.ones((rows, width), f32)
    for lag in range(1, props):
        later = later * jnp.where(
            at < props - lag, pltpu.roll(decay, rows - lag, axis=0), 1.0
        )
    enter = enter * later
    whole = jnp.where(at == 0, decay * later, 0.0)

    def split(x):
        high = x.astype(bf16).astype(f32)
        return high, x - high

    coeffs = jnp.concatenate(split(enter) + split(whole), axis=0)
    seq_row = lax.div(
        lax.rem(lax.broadcasted_iota(jnp.int32, (2 * rows, HEAD_DIM), 0), rows), props
    )
    nothing = jnp.zeros((2 * rows, HEAD_DIM), f32)
    left, values = [], []
    for h in range(head_local):
        part = slice(h * HEAD_DIM, (h + 1) * HEAD_DIM)
        left.append(coeffs[:, part].T.astype(bf16))
        values.append(jnp.concatenate([prev_v[:, part]] * 2, axis=0))

    def take(s, carry):
        own = seq_row == s
        for h in range(head_local):
            right = jnp.concatenate(
                [
                    jnp.concatenate([jnp.where(own, values[h], 0.0), nothing], axis=1),
                    jnp.concatenate([nothing, jnp.where(own, 1.0, 0.0)], axis=1),
                ],
                axis=0,
            ).astype(bf16)
            both = jnp.dot(left[h], right, preferred_element_type=f32)
            fresh = both[:, HEAD_DIM:] * state[s, h] + both[:, :HEAD_DIM]
            state[s, h] = fresh
            state16[h, :, pl.ds(pl.multiple_of(s * HEAD_DIM, HEAD_DIM), HEAD_DIM)] = fresh.astype(
                bf16
            )
        return carry

    lax.fori_loop(0, seqs, take, 0)
    taken_copy = pltpu.make_async_copy(state, taken, taken_sem)
    taken_copy.start()
    for copy in locals_[5:]:
        copy.wait()

    def project(source, block, first):
        x = block.astype(f32).reshape(rows, cols)
        lanes = pl.ds(pl.multiple_of(source * cols, cols), cols)
        scaled = (x * gain_v[:, lanes]).astype(bf16)
        term = jnp.dot(scaled, w_all[lanes, :], preferred_element_type=f32)
        if first:
            acc[...] = term
        else:
            acc[...] += term
        return jnp.sum(x * x, axis=1, keepdims=True)

    squares = project(kv, hid[pl.ds(kv * seqs, seqs)], True)
    fwd_copies = {}
    for place, step in enumerate(order):
        source = lax.rem(kv + n_kv - step, n_kv)
        in_copies[step].wait_recv()
        fwd_copies[step] = remote(
            arrived.at[source, mine],
            arrived.at[source, mine],
            fwd_send.at[step],
            fwd_recv.at[step],
            {"tp": peer},
        )
        fwd_copies[step].start()
        if place:
            step = order[place - 1]
            source = lax.rem(kv + n_kv - step, n_kv)
            fwd_copies[step].wait_recv()
            squares += project(source, arrived[source], False)
    step = order[-1]
    source = lax.rem(kv + n_kv - step, n_kv)
    fwd_copies[step].wait_recv()
    squares += project(source, arrived[source], False)

    scale = lax.rsqrt(squares / depth + 1e-06)
    pre = [
        (acc[:, place * width : (place + 1) * width] * scale).astype(bf16).astype(f32)
        for place in range(4)
    ]
    query = jax.nn.silu(pre[0])
    forget = low + (1.0 - low) * jax.nn.sigmoid(pre[1])
    key = 1.0 - forget
    value = pre[2]
    gate = jax.nn.silu(pre[3])
    shifted = [forget] + [pltpu.roll(forget, lag, axis=0) for lag in range(1, props)]
    reach = forget
    for lag in range(1, props):
        reach = reach * jnp.where(at >= lag, shifted[lag], 1.0)
    from_state = (query * reach).astype(bf16)
    near = []
    walk = query
    for lag in range(props):
        if lag:
            walk = walk * shifted[lag - 1]
            near.append(
                (
                    jnp.where(at >= lag, walk * pltpu.roll(key, lag, axis=0), 0.0),
                    pltpu.roll(value, lag, axis=0),
                )
            )
        else:
            near.append((walk * key, value))
    seq_head = lax.div(lax.broadcasted_iota(jnp.int32, (rows, HEAD_DIM), 0), props)
    for h in range(head_local):
        part = slice(h * HEAD_DIM, (h + 1) * HEAD_DIM)
        every = jnp.dot(from_state[:, part], state16[h], preferred_element_type=f32)
        o = jnp.zeros((rows, HEAD_DIM), f32)
        for s in range(seqs):
            o = jnp.where(seq_head == s, every[:, s * HEAD_DIM : (s + 1) * HEAD_DIM], o)
        for weight, fresh in near:
            o += jnp.sum(weight[:, part], axis=1, keepdims=True) * fresh[:, part]
        size = lax.rsqrt(jnp.mean(o * o, axis=1, keepdims=True) + 1e-05)
        heads_all[tp, :, part] = (o * size * head_gain_v[...] * gate[:, part]).astype(bf16)

    tp_copies = {}
    for step in sorted(range(1, n_tp), key=lambda step: -step % 2):
        to = lax.rem(tp + step, n_tp)
        tp_copies[step] = remote(
            heads_all.at[tp], heads_all.at[tp], tp_send.at[step], tp_recv.at[step], {"tp": to}
        )
        tp_copies[step].start()
    for copy in w_o_copies:
        copy.wait()

    def mix(owner):
        lines = pl.ds(pl.multiple_of(owner * width, width), width)
        return jnp.dot(heads_all[owner], w_o[lines, :], preferred_element_type=f32)

    acc_out = mix(tp)
    for step, copy in tp_copies.items():
        copy.wait_recv()
        acc_out += mix(lax.rem(tp + n_tp - step, n_tp))
    for k in range(n_kv):
        blocks[k] = acc_out[:, k * half_cols : (k + 1) * half_cols].astype(bf16)

    out_copies = {}
    for step in order:
        to = lax.rem(kv + step, n_kv)
        out_copies[step] = remote(
            blocks.at[to], landed.at[kv, core], out_send.at[step], out_recv.at[step], {"kv": to}
        )
        out_copies[step].start()
    ofwd = {
        0: remote(
            blocks.at[kv], landed.at[kv, core], ofwd_send.at[0], ofwd_recv.at[0], {"tp": peer}
        )
    }
    ofwd[0].start()
    landed[kv, core] = blocks[kv]
    for step in order:
        source = lax.rem(kv + n_kv - step, n_kv)
        out_copies[step].wait_recv()
        ofwd[step] = remote(
            landed.at[source, core],
            landed.at[source, core],
            ofwd_send.at[step],
            ofwd_recv.at[step],
            {"tp": peer},
        )
        ofwd[step].start()
    for copy in ofwd.values():
        copy.wait_recv()
    for k in range(n_kv):
        out[k * rows : (k + 1) * rows, :] = jnp.concatenate([landed[k, 0], landed[k, 1]], axis=1)
    for group in (in_copies, fwd_copies, tp_copies, out_copies, ofwd):
        for copy in group.values():
            copy.wait_send()
    taken_copy.wait()


def fused(
    n_kv,
    n_tp,
    hidden,
    norm_gain,
    w_query,
    w_forget,
    w_input,
    w_outgate,
    w_out,
    floor,
    head_gain,
    base_state,
    prev_forget,
    prev_input,
    accepted,
):
    f32, bf16 = jnp.float32, jnp.bfloat16
    all_seqs, props, cols = hidden.shape
    seqs = all_seqs // n_kv
    rows = seqs * props
    width = w_query.shape[1]
    depth = n_kv * cols
    head_local = width // HEAD_DIM
    anywhere = pl.BlockSpec(memory_space=pl.ANY)
    dma = pltpu.SemaphoreType.DMA
    out, taken = pl.pallas_call(
        functools.partial(fused_kernel, n_kv, n_tp),
        out_shape=(
            jax.ShapeDtypeStruct((all_seqs * props, cols), bf16),
            jax.ShapeDtypeStruct(base_state.shape, f32),
        ),
        in_specs=[pl.BlockSpec(memory_space=pltpu.SMEM)] + [anywhere] * 12,
        out_specs=(pl.BlockSpec(memory_space=pltpu.VMEM), anywhere),
        scratch_shapes=[
            pltpu.VMEM(hidden.shape, bf16),
            pltpu.VMEM((n_kv, seqs, props, cols), bf16),
            pltpu.VMEM((1, depth), f32),
            pltpu.VMEM((depth, 4 * width), bf16),
            pltpu.VMEM((n_tp * width, depth // 2), bf16),
            pltpu.VMEM((1, width), f32),
            pltpu.VMEM((1, HEAD_DIM), f32),
            pltpu.VMEM(base_state.shape, f32),
            pltpu.VMEM((head_local, HEAD_DIM, seqs * HEAD_DIM), bf16),
            pltpu.VMEM(prev_forget.shape, bf16),
            pltpu.VMEM(prev_input.shape, bf16),
            pltpu.VMEM((rows, 4 * width), f32),
            pltpu.VMEM((n_tp, rows, width), bf16),
            pltpu.VMEM((n_kv, rows, cols // 2), bf16),
            pltpu.VMEM((n_kv, 2, rows, cols // 2), bf16),
            dma((11,)),
            dma((n_kv,)),
            dma,
            dma((n_kv,)),
            dma((n_kv,)),
            dma((n_kv,)),
            dma((n_kv,)),
            dma((n_tp,)),
            dma((n_tp,)),
            dma((n_kv,)),
            dma((n_kv,)),
            dma((n_kv,)),
            dma((n_kv,)),
        ],
        compiler_params=pltpu.CompilerParams(
            collective_id=0, has_side_effects=True, vmem_limit_bytes=56 * 1024 * 1024
        ),
    )(
        accepted,
        hidden,
        norm_gain.reshape(1, depth),
        w_query,
        w_forget,
        w_input,
        w_outgate,
        w_out,
        floor.reshape(1, width),
        head_gain.reshape(1, HEAD_DIM),
        base_state,
        prev_forget,
        prev_input,
    )
    return out.reshape(hidden.shape), taken


def by_shape(n_kv, n_tp, hidden, *rest):
    if hidden.shape[2] % 256 == 0 and n_tp % 2 == 0:
        return fused(n_kv, n_tp, hidden, *rest)
    return shards(hidden, *rest)


def solution(mesh):
    placed = (
        P(None, None, "kv"),
        P(),
        P(None, "tp"),
        P(None, "tp"),
        P(None, "tp"),
        P(None, "tp"),
        P(),
        P("tp"),
        P(),
        P("kv", "tp", None, None),
        P("kv", None, "tp"),
        P("kv", None, "tp"),
        P("kv"),
    )
    return jax.shard_map(
        functools.partial(by_shape, mesh.shape["kv"], mesh.shape["tp"]),
        mesh=mesh,
        in_specs=placed,
        out_specs=(P(None, None, "kv"), P("kv", "tp", None, None)),
        check_vma=False,
    )
```

```python
import functools

import jax
import jax.numpy as jnp
from jax import lax
from jax.experimental import pallas as pl
from jax.experimental.pallas import tpu as pltpu
from jax.sharding import PartitionSpec as P

D = 2048
HEAD_DIM = 128
PROPS = 4


def shards(
    hidden,
    norm_gain,
    w_query,
    w_forget,
    w_input,
    w_outgate,
    w_out,
    floor,
    head_gain,
    base_state,
    prev_forget,
    prev_input,
    accepted,
):
    arrived = lax.all_to_all(hidden, "kv", split_axis=0, concat_axis=2, tiled=True)
    whole_vals = arrived.astype(jnp.float32)
    row_sums = jnp.sum(whole_vals * whole_vals, axis=2)
    normed = (whole_vals * lax.rsqrt(row_sums / D + 1e-06)[..., None] * norm_gain).astype(
        jnp.bfloat16
    )
    query_pre = jnp.dot(normed, w_query, preferred_element_type=jnp.float32).astype(jnp.bfloat16)
    forget_pre = jnp.dot(normed, w_forget, preferred_element_type=jnp.float32).astype(jnp.bfloat16)
    input_pre = jnp.dot(normed, w_input, preferred_element_type=jnp.float32).astype(jnp.bfloat16)
    gate_pre = jnp.dot(normed, w_outgate, preferred_element_type=jnp.float32).astype(jnp.bfloat16)
    seq_local = normed.shape[0]
    head_local = w_query.shape[1] // HEAD_DIM
    shape = (seq_local, PROPS, head_local, HEAD_DIM)
    query = jax.nn.silu(query_pre.astype(jnp.float32)).reshape(shape)
    forget = (floor + (1.0 - floor) * jax.nn.sigmoid(forget_pre.astype(jnp.float32))).reshape(shape)
    value = input_pre.astype(jnp.float32).reshape(shape)
    prev_f = (floor + (1.0 - floor) * jax.nn.sigmoid(prev_forget.astype(jnp.float32))).reshape(
        shape
    )
    prev_v = prev_input.astype(jnp.float32).reshape(shape)
    state = base_state
    for step in range(PROPS):
        live = (step < accepted)[:, None, None, None]
        moved = (
            prev_f[:, step][..., None] * state
            + (1.0 - prev_f[:, step])[..., None] * prev_v[:, step][:, :, None, :]
        )
        state = jnp.where(live, moved, state)
    taken_state = state
    outputs = []
    for step in range(PROPS):
        state = (
            forget[:, step][..., None] * state
            + (1.0 - forget[:, step])[..., None] * value[:, step][:, :, None, :]
        )
        outputs.append(
            jnp.einsum("bhk,bhkv->bhv", query[:, step], state, precision=lax.Precision.HIGHEST)
        )
    result = jnp.stack(outputs, axis=1)
    scaled = (
        result * lax.rsqrt(jnp.mean(result * result, axis=-1, keepdims=True) + 1e-05) * head_gain
    )
    gated = scaled * jax.nn.silu(gate_pre.astype(jnp.float32)).reshape(shape)
    mixed_heads = gated.reshape(seq_local, PROPS, head_local * HEAD_DIM).astype(jnp.bfloat16)
    own_rows = mixed_heads.shape[2]
    w_rows = lax.dynamic_slice_in_dim(w_out, lax.axis_index("tp") * own_rows, own_rows, 0)
    partial_value = jnp.dot(mixed_heads, w_rows, preferred_element_type=jnp.float32)
    finished = lax.psum(partial_value, "tp").astype(jnp.bfloat16)
    mixed = lax.all_to_all(finished, "kv", split_axis=2, concat_axis=0, tiled=True)
    return (mixed, taken_state)


def fused_kernel(
    n_kv,
    n_tp,
    accepted_hbm,
    hidden,
    gain,
    w_query,
    w_forget,
    w_input,
    w_outgate,
    w_out,
    floor,
    head_gain,
    base_state,
    prev_forget,
    prev_input,
    out,
    taken,
    hid,
    arrived,
    gain_v,
    w_all,
    w_o,
    floor_v,
    head_gain_v,
    state,
    state16,
    prev_f_v,
    prev_i_v,
    counts,
    acc,
    heads_all,
    blocks,
    landed,
    local_sem,
    wo_sem,
    in_send,
    in_recv,
    fwd_send,
    fwd_recv,
    tp_send,
    tp_recv,
    out_send,
    out_recv,
    ofwd_send,
    ofwd_recv,
):
    f32, bf16 = jnp.float32, jnp.bfloat16
    seqs, props = hid.shape[0] // n_kv, hid.shape[1]
    cols = hid.shape[2]
    rows = seqs * props
    half_seq = seqs // 2
    width = w_query.shape[1]
    head_local = width // HEAD_DIM
    half_cols = cols // 2
    depth = n_kv * cols
    kv, tp = lax.axis_index("kv"), lax.axis_index("tp")
    core = lax.rem(tp, 2)
    peer = tp + 1 - 2 * core

    locals_ = [
        pltpu.make_async_copy(hidden, hid, local_sem.at[0]),
        pltpu.make_async_copy(prev_forget, prev_f_v, local_sem.at[1]),
        pltpu.make_async_copy(prev_input, prev_i_v, local_sem.at[2]),
        pltpu.make_async_copy(floor, floor_v, local_sem.at[3]),
        pltpu.make_async_copy(base_state, state, local_sem.at[4]),
        pltpu.make_async_copy(accepted_hbm, counts, local_sem.at[11]),
        pltpu.make_async_copy(gain, gain_v, local_sem.at[5]),
        pltpu.make_async_copy(head_gain, head_gain_v, local_sem.at[6]),
    ]
    for place, weight in enumerate((w_query, w_forget, w_input, w_outgate)):
        locals_.append(
            pltpu.make_async_copy(
                weight, w_all.at[:, pl.ds(place * width, width)], local_sem.at[7 + place]
            )
        )
    w_o_copies = [
        pltpu.make_async_copy(
            w_out.at[:, pl.ds(pl.multiple_of(k * cols + core * half_cols, half_cols), half_cols)],
            w_o.at[:, pl.ds(k * half_cols, half_cols)],
            wo_sem.at[k],
        )
        for k in range(n_kv)
    ]
    barrier = pltpu.get_barrier_semaphore()
    for step in range(1, n_kv):
        pl.semaphore_signal(
            barrier,
            inc=1,
            device_id={"kv": lax.rem(kv + step, n_kv)},
            device_id_type=pl.DeviceIdType.MESH,
        )
    for step in range(1, n_tp):
        pl.semaphore_signal(
            barrier,
            inc=1,
            device_id={"tp": lax.rem(tp + step, n_tp)},
            device_id_type=pl.DeviceIdType.MESH,
        )
    for copy in locals_:
        copy.start()
    for copy in w_o_copies:
        copy.start()
    locals_[0].wait()
    pl.semaphore_wait(barrier, n_kv + n_tp - 2)

    def remote(source, target, send, recv, device):
        return pltpu.make_async_remote_copy(
            src_ref=source,
            dst_ref=target,
            send_sem=send,
            recv_sem=recv,
            device_id=device,
            device_id_type=pl.DeviceIdType.MESH,
        )

    order = sorted(range(1, n_kv), key=lambda step: -min(step, n_kv - step))
    mine = pl.ds(core * half_seq, half_seq)
    in_copies = {}
    for step in order:
        to = lax.rem(kv + step, n_kv)
        in_copies[step] = remote(
            hid.at[pl.ds(to * seqs + core * half_seq, half_seq)],
            arrived.at[kv, mine],
            in_send.at[step],
            in_recv.at[step],
            {"kv": to},
        )
        in_copies[step].start()

    for copy in locals_[1:6]:
        copy.wait()
    low = floor_v[...]
    row = lax.broadcasted_iota(jnp.int32, (rows, width), 0)
    at = lax.rem(row, props)
    seq_of = lax.div(row, props)
    taken_count = jnp.zeros((rows, width), jnp.int32)
    for s in range(seqs):
        taken_count = jnp.where(seq_of == s, counts[s], taken_count)
    live = at < taken_count
    prev_f = low + (1.0 - low) * jax.nn.sigmoid(
        prev_f_v[...].astype(f32).reshape(rows, width)
    )
    prev_v = prev_i_v[...].astype(f32).reshape(rows, width)
    decay = jnp.where(live, prev_f, 1.0)
    enter = jnp.where(live, 1.0 - prev_f, 0.0)
    later = jnp.ones((rows, width), f32)
    for lag in range(1, props):
        later = later * jnp.where(
            at < props - lag, pltpu.roll(decay, rows - lag, axis=0), 1.0
        )
    enter = enter * later
    whole = jnp.where(at == 0, decay * later, 0.0)

    def split(x):
        high = x.astype(bf16).astype(f32)
        return high, x - high

    coeffs = jnp.concatenate(split(enter) + split(whole), axis=0)
    seq_row = lax.div(
        lax.rem(lax.broadcasted_iota(jnp.int32, (2 * rows, HEAD_DIM), 0), rows), props
    )
    nothing = jnp.zeros((2 * rows, HEAD_DIM), f32)
    left, values = [], []
    for h in range(head_local):
        part = slice(h * HEAD_DIM, (h + 1) * HEAD_DIM)
        left.append(coeffs[:, part].T.astype(bf16))
        values.append(jnp.concatenate([prev_v[:, part]] * 2, axis=0))

    def take(s, carry):
        own = seq_row == s
        for h in range(head_local):
            right = jnp.concatenate(
                [
                    jnp.concatenate([jnp.where(own, values[h], 0.0), nothing], axis=1),
                    jnp.concatenate([nothing, jnp.where(own, 1.0, 0.0)], axis=1),
                ],
                axis=0,
            ).astype(bf16)
            both = jnp.dot(left[h], right, preferred_element_type=f32)
            fresh = both[:, HEAD_DIM:] * state[s, h] + both[:, :HEAD_DIM]
            taken[s, h] = fresh
            state16[h, :, pl.ds(pl.multiple_of(s * HEAD_DIM, HEAD_DIM), HEAD_DIM)] = fresh.astype(
                bf16
            )
        return carry

    lax.fori_loop(0, seqs, take, 0)
    for copy in locals_[6:]:
        copy.wait()

    def project(source, block, first):
        x = block.astype(f32).reshape(rows, cols)
        lanes = pl.ds(pl.multiple_of(source * cols, cols), cols)
        scaled = (x * gain_v[:, lanes]).astype(bf16)
        term = jnp.dot(scaled, w_all[lanes, :], preferred_element_type=f32)
        if first:
            acc[...] = term
        else:
            acc[...] += term
        return jnp.sum(x * x, axis=1, keepdims=True)

    squares = project(kv, hid[pl.ds(kv * seqs, seqs)], True)
    fwd_copies = {}
    for place, step in enumerate(order):
        source = lax.rem(kv + n_kv - step, n_kv)
        in_copies[step].wait_recv()
        fwd_copies[step] = remote(
            arrived.at[source, mine],
            arrived.at[source, mine],
            fwd_send.at[step],
            fwd_recv.at[step],
            {"tp": peer},
        )
        fwd_copies[step].start()
        if place:
            step = order[place - 1]
            source = lax.rem(kv + n_kv - step, n_kv)
            fwd_copies[step].wait_recv()
            squares += project(source, arrived[source], False)
    step = order[-1]
    source = lax.rem(kv + n_kv - step, n_kv)
    fwd_copies[step].wait_recv()
    squares += project(source, arrived[source], False)

    scale = lax.rsqrt(squares / depth + 1e-06)
    pre = [
        (acc[:, place * width : (place + 1) * width] * scale).astype(bf16).astype(f32)
        for place in range(4)
    ]
    query = jax.nn.silu(pre[0])
    forget = low + (1.0 - low) * jax.nn.sigmoid(pre[1])
    key = 1.0 - forget
    value = pre[2]
    gate = jax.nn.silu(pre[3])
    shifted = [forget] + [pltpu.roll(forget, lag, axis=0) for lag in range(1, props)]
    reach = forget
    for lag in range(1, props):
        reach = reach * jnp.where(at >= lag, shifted[lag], 1.0)
    from_state = (query * reach).astype(bf16)
    near = []
    walk = query
    for lag in range(props):
        if lag:
            walk = walk * shifted[lag - 1]
            near.append(
                (
                    jnp.where(at >= lag, walk * pltpu.roll(key, lag, axis=0), 0.0),
                    pltpu.roll(value, lag, axis=0),
                )
            )
        else:
            near.append((walk * key, value))
    seq_head = lax.div(lax.broadcasted_iota(jnp.int32, (rows, HEAD_DIM), 0), props)
    for h in range(head_local):
        part = slice(h * HEAD_DIM, (h + 1) * HEAD_DIM)
        every = jnp.dot(from_state[:, part], state16[h], preferred_element_type=f32)
        o = jnp.zeros((rows, HEAD_DIM), f32)
        for s in range(seqs):
            o = jnp.where(seq_head == s, every[:, s * HEAD_DIM : (s + 1) * HEAD_DIM], o)
        for weight, fresh in near:
            o += jnp.sum(weight[:, part], axis=1, keepdims=True) * fresh[:, part]
        size = lax.rsqrt(jnp.mean(o * o, axis=1, keepdims=True) + 1e-05)
        heads_all[tp, :, part] = (o * size * head_gain_v[...] * gate[:, part]).astype(bf16)

    tp_copies = {}
    for step in sorted(range(1, n_tp), key=lambda step: -step % 2):
        to = lax.rem(tp + step, n_tp)
        tp_copies[step] = remote(
            heads_all.at[tp], heads_all.at[tp], tp_send.at[step], tp_recv.at[step], {"tp": to}
        )
        tp_copies[step].start()
    for copy in w_o_copies:
        copy.wait()

    def mix(owner):
        lines = pl.ds(pl.multiple_of(owner * width, width), width)
        return jnp.dot(heads_all[owner], w_o[lines, :], preferred_element_type=f32)

    acc_out = mix(tp)
    for step, copy in tp_copies.items():
        copy.wait_recv()
        acc_out += mix(lax.rem(tp + n_tp - step, n_tp))
    for k in range(n_kv):
        blocks[k] = acc_out[:, k * half_cols : (k + 1) * half_cols].astype(bf16)

    out_copies = {}
    for step in order:
        to = lax.rem(kv + step, n_kv)
        out_copies[step] = remote(
            blocks.at[to], landed.at[kv, core], out_send.at[step], out_recv.at[step], {"kv": to}
        )
        out_copies[step].start()
    ofwd = {
        0: remote(
            blocks.at[kv], landed.at[kv, core], ofwd_send.at[0], ofwd_recv.at[0], {"tp": peer}
        )
    }
    ofwd[0].start()
    landed[kv, core] = blocks[kv]
    for step in order:
        source = lax.rem(kv + n_kv - step, n_kv)
        out_copies[step].wait_recv()
        ofwd[step] = remote(
            landed.at[source, core],
            landed.at[source, core],
            ofwd_send.at[step],
            ofwd_recv.at[step],
            {"tp": peer},
        )
        ofwd[step].start()
    for copy in ofwd.values():
        copy.wait_recv()
    for k in range(n_kv):
        out[k * rows : (k + 1) * rows, :] = jnp.concatenate([landed[k, 0], landed[k, 1]], axis=1)
    for group in (in_copies, fwd_copies, tp_copies, out_copies, ofwd):
        for copy in group.values():
            copy.wait_send()


def write_kernel(flat, taken, out, stored, sem):
    copy = pltpu.make_async_copy(taken, stored, sem)
    copy.start()
    out[...] = flat[...].astype(jnp.float32).reshape(out.shape).astype(out.dtype)
    copy.wait()


def fused(
    n_kv,
    n_tp,
    hidden,
    norm_gain,
    w_query,
    w_forget,
    w_input,
    w_outgate,
    w_out,
    floor,
    head_gain,
    base_state,
    prev_forget,
    prev_input,
    accepted,
):
    f32, bf16 = jnp.float32, jnp.bfloat16
    all_seqs, props, cols = hidden.shape
    seqs = all_seqs // n_kv
    rows = seqs * props
    width = w_query.shape[1]
    depth = n_kv * cols
    head_local = width // HEAD_DIM
    anywhere = pl.BlockSpec(memory_space=pl.ANY)
    dma = pltpu.SemaphoreType.DMA
    room = 67043328 - base_state.size * 4 - hidden.size * 2 - 64 * 1024
    out, taken = pl.pallas_call(
        functools.partial(fused_kernel, n_kv, n_tp),
        out_shape=(
            pltpu.VMEM((all_seqs * props, cols), bf16),
            pltpu.VMEM(base_state.shape, f32),
        ),
        in_specs=[anywhere] * 13,
        out_specs=(pl.BlockSpec(memory_space=pltpu.VMEM),) * 2,
        scratch_shapes=[
            pltpu.VMEM(hidden.shape, bf16),
            pltpu.VMEM((n_kv, seqs, props, cols), bf16),
            pltpu.VMEM((1, depth), f32),
            pltpu.VMEM((depth, 4 * width), bf16),
            pltpu.VMEM((n_tp * width, depth // 2), bf16),
            pltpu.VMEM((1, width), f32),
            pltpu.VMEM((1, HEAD_DIM), f32),
            pltpu.VMEM(base_state.shape, f32),
            pltpu.VMEM((head_local, HEAD_DIM, seqs * HEAD_DIM), bf16),
            pltpu.VMEM(prev_forget.shape, bf16),
            pltpu.VMEM(prev_input.shape, bf16),
            pltpu.SMEM(accepted.shape, jnp.int32),
            pltpu.VMEM((rows, 4 * width), f32),
            pltpu.VMEM((n_tp, rows, width), bf16),
            pltpu.VMEM((n_kv, rows, cols // 2), bf16),
            pltpu.VMEM((n_kv, 2, rows, cols // 2), bf16),
            dma((12,)),
            dma((n_kv,)),
            dma((n_kv,)),
            dma((n_kv,)),
            dma((n_kv,)),
            dma((n_kv,)),
            dma((n_tp,)),
            dma((n_tp,)),
            dma((n_kv,)),
            dma((n_kv,)),
            dma((n_kv,)),
            dma((n_kv,)),
        ],
        compiler_params=pltpu.CompilerParams(
            collective_id=0, has_side_effects=True, vmem_limit_bytes=room
        ),
    )(
        accepted,
        hidden,
        norm_gain.reshape(1, depth),
        w_query,
        w_forget,
        w_input,
        w_outgate,
        w_out,
        floor.reshape(1, width),
        head_gain.reshape(1, HEAD_DIM),
        base_state,
        prev_forget,
        prev_input,
    )
    return pl.pallas_call(
        write_kernel,
        out_shape=(
            jax.ShapeDtypeStruct(hidden.shape, bf16),
            jax.ShapeDtypeStruct(base_state.shape, f32),
        ),
        in_specs=[pl.BlockSpec(memory_space=pltpu.VMEM)] * 2,
        out_specs=(pl.BlockSpec(memory_space=pltpu.VMEM), anywhere),
        scratch_shapes=[dma],
        compiler_params=pltpu.CompilerParams(vmem_limit_bytes=16 * 1024 * 1024),
    )(out, taken)


def by_shape(n_kv, n_tp, hidden, *rest):
    if hidden.shape[2] % 256 == 0 and n_tp % 2 == 0:
        return fused(n_kv, n_tp, hidden, *rest)
    return shards(hidden, *rest)


def solution(mesh):
    placed = (
        P(None, None, "kv"),
        P(),
        P(None, "tp"),
        P(None, "tp"),
        P(None, "tp"),
        P(None, "tp"),
        P(),
        P("tp"),
        P(),
        P("kv", "tp", None, None),
        P("kv", None, "tp"),
        P("kv", None, "tp"),
        P("kv"),
    )
    return jax.shard_map(
        functools.partial(by_shape, mesh.shape["kv"], mesh.shape["tp"]),
        mesh=mesh,
        in_specs=placed,
        out_specs=(P(None, None, "kv"), P("kv", "tp", None, None)),
        check_vma=False,
    )
```

```python
import functools

import jax
import jax.numpy as jnp
from jax import lax
from jax.experimental import pallas as pl
from jax.experimental.pallas import tpu as pltpu
from jax.sharding import PartitionSpec as P

D = 2048
HEAD_DIM = 128
PROPS = 4


def shards(
    hidden,
    norm_gain,
    w_query,
    w_forget,
    w_input,
    w_outgate,
    w_out,
    floor,
    head_gain,
    base_state,
    prev_forget,
    prev_input,
    accepted,
):
    arrived = lax.all_to_all(hidden, "kv", split_axis=0, concat_axis=2, tiled=True)
    whole_vals = arrived.astype(jnp.float32)
    row_sums = jnp.sum(whole_vals * whole_vals, axis=2)
    normed = (whole_vals * lax.rsqrt(row_sums / D + 1e-06)[..., None] * norm_gain).astype(
        jnp.bfloat16
    )
    query_pre = jnp.dot(normed, w_query, preferred_element_type=jnp.float32).astype(jnp.bfloat16)
    forget_pre = jnp.dot(normed, w_forget, preferred_element_type=jnp.float32).astype(jnp.bfloat16)
    input_pre = jnp.dot(normed, w_input, preferred_element_type=jnp.float32).astype(jnp.bfloat16)
    gate_pre = jnp.dot(normed, w_outgate, preferred_element_type=jnp.float32).astype(jnp.bfloat16)
    seq_local = normed.shape[0]
    head_local = w_query.shape[1] // HEAD_DIM
    shape = (seq_local, PROPS, head_local, HEAD_DIM)
    query = jax.nn.silu(query_pre.astype(jnp.float32)).reshape(shape)
    forget = (floor + (1.0 - floor) * jax.nn.sigmoid(forget_pre.astype(jnp.float32))).reshape(shape)
    value = input_pre.astype(jnp.float32).reshape(shape)
    prev_f = (floor + (1.0 - floor) * jax.nn.sigmoid(prev_forget.astype(jnp.float32))).reshape(
        shape
    )
    prev_v = prev_input.astype(jnp.float32).reshape(shape)
    state = base_state
    for step in range(PROPS):
        live = (step < accepted)[:, None, None, None]
        moved = (
            prev_f[:, step][..., None] * state
            + (1.0 - prev_f[:, step])[..., None] * prev_v[:, step][:, :, None, :]
        )
        state = jnp.where(live, moved, state)
    taken_state = state
    outputs = []
    for step in range(PROPS):
        state = (
            forget[:, step][..., None] * state
            + (1.0 - forget[:, step])[..., None] * value[:, step][:, :, None, :]
        )
        outputs.append(
            jnp.einsum("bhk,bhkv->bhv", query[:, step], state, precision=lax.Precision.HIGHEST)
        )
    result = jnp.stack(outputs, axis=1)
    scaled = (
        result * lax.rsqrt(jnp.mean(result * result, axis=-1, keepdims=True) + 1e-05) * head_gain
    )
    gated = scaled * jax.nn.silu(gate_pre.astype(jnp.float32)).reshape(shape)
    mixed_heads = gated.reshape(seq_local, PROPS, head_local * HEAD_DIM).astype(jnp.bfloat16)
    own_rows = mixed_heads.shape[2]
    w_rows = lax.dynamic_slice_in_dim(w_out, lax.axis_index("tp") * own_rows, own_rows, 0)
    partial_value = jnp.dot(mixed_heads, w_rows, preferred_element_type=jnp.float32)
    finished = lax.psum(partial_value, "tp").astype(jnp.bfloat16)
    mixed = lax.all_to_all(finished, "kv", split_axis=2, concat_axis=0, tiled=True)
    return (mixed, taken_state)


def fused_kernel(
    n_kv,
    n_tp,
    accepted_hbm,
    hidden,
    gain,
    w_query,
    w_forget,
    w_input,
    w_outgate,
    w_out,
    floor,
    head_gain,
    base_state,
    prev_forget,
    prev_input,
    out,
    taken,
    hid,
    arrived,
    gain_v,
    w_all,
    w_o,
    floor_v,
    head_gain_v,
    state,
    state16,
    prev_f_v,
    prev_i_v,
    counts,
    acc,
    heads_all,
    blocks,
    landed,
    local_sem,
    wo_sem,
    in_send,
    in_recv,
    fwd_send,
    fwd_recv,
    tp_send,
    tp_recv,
    out_send,
    out_recv,
    ofwd_send,
    ofwd_recv,
):
    f32, bf16 = jnp.float32, jnp.bfloat16
    seqs, props = hid.shape[0] // n_kv, hid.shape[1]
    cols = hid.shape[2]
    rows = seqs * props
    half_seq = seqs // 2
    width = w_query.shape[1]
    head_local = width // HEAD_DIM
    half_cols = cols // 2
    depth = n_kv * cols
    kv, tp = lax.axis_index("kv"), lax.axis_index("tp")
    core = lax.rem(tp, 2)
    peer = tp + 1 - 2 * core

    locals_ = [
        pltpu.make_async_copy(hidden, hid, local_sem.at[0]),
        pltpu.make_async_copy(prev_forget, prev_f_v, local_sem.at[1]),
        pltpu.make_async_copy(prev_input, prev_i_v, local_sem.at[2]),
        pltpu.make_async_copy(floor, floor_v, local_sem.at[3]),
        pltpu.make_async_copy(base_state, state, local_sem.at[4]),
        pltpu.make_async_copy(accepted_hbm, counts, local_sem.at[11]),
        pltpu.make_async_copy(gain, gain_v, local_sem.at[5]),
        pltpu.make_async_copy(head_gain, head_gain_v, local_sem.at[6]),
    ]
    for place, weight in enumerate((w_query, w_forget, w_input, w_outgate)):
        locals_.append(
            pltpu.make_async_copy(
                weight, w_all.at[:, pl.ds(place * width, width)], local_sem.at[7 + place]
            )
        )
    w_o_copies = [
        pltpu.make_async_copy(
            w_out.at[:, pl.ds(pl.multiple_of(k * cols + core * half_cols, half_cols), half_cols)],
            w_o.at[:, pl.ds(k * half_cols, half_cols)],
            wo_sem.at[k],
        )
        for k in range(n_kv)
    ]
    locals_[0].start()
    barrier = pltpu.get_barrier_semaphore()
    for step in range(1, n_kv):
        pl.semaphore_signal(
            barrier,
            inc=1,
            device_id={"kv": lax.rem(kv + step, n_kv)},
            device_id_type=pl.DeviceIdType.MESH,
        )
    for step in range(1, n_tp):
        pl.semaphore_signal(
            barrier,
            inc=1,
            device_id={"tp": lax.rem(tp + step, n_tp)},
            device_id_type=pl.DeviceIdType.MESH,
        )
    for copy in locals_[1:]:
        copy.start()
    for copy in w_o_copies:
        copy.start()
    locals_[0].wait()
    pl.semaphore_wait(barrier, n_kv + n_tp - 2)

    def remote(source, target, send, recv, device):
        return pltpu.make_async_remote_copy(
            src_ref=source,
            dst_ref=target,
            send_sem=send,
            recv_sem=recv,
            device_id=device,
            device_id_type=pl.DeviceIdType.MESH,
        )

    order = sorted(range(1, n_kv), key=lambda step: -min(step, n_kv - step))
    mine = pl.ds(core * half_seq, half_seq)
    in_copies = {}
    for step in order:
        to = lax.rem(kv + step, n_kv)
        in_copies[step] = remote(
            hid.at[pl.ds(to * seqs + core * half_seq, half_seq)],
            arrived.at[kv, mine],
            in_send.at[step],
            in_recv.at[step],
            {"kv": to},
        )
        in_copies[step].start()

    for copy in locals_[1:6]:
        copy.wait()
    low = floor_v[...]
    row = lax.broadcasted_iota(jnp.int32, (rows, width), 0)
    at = lax.rem(row, props)
    seq_of = lax.div(row, props)
    taken_count = jnp.zeros((rows, width), jnp.int32)
    for s in range(seqs):
        taken_count = jnp.where(seq_of == s, counts[s], taken_count)
    live = at < taken_count
    prev_f = low + (1.0 - low) * jax.nn.sigmoid(
        prev_f_v[...].astype(f32).reshape(rows, width)
    )
    prev_v = prev_i_v[...].astype(f32).reshape(rows, width)
    decay = jnp.where(live, prev_f, 1.0)
    enter = jnp.where(live, 1.0 - prev_f, 0.0)
    later = jnp.ones((rows, width), f32)
    for lag in range(1, props):
        later = later * jnp.where(
            at < props - lag, pltpu.roll(decay, rows - lag, axis=0), 1.0
        )
    enter = enter * later
    whole = jnp.where(at == 0, decay * later, 0.0)

    def split(x):
        high = x.astype(bf16).astype(f32)
        return high, x - high

    coeffs = jnp.concatenate(split(enter) + split(whole), axis=0)
    seq_row = lax.div(
        lax.rem(lax.broadcasted_iota(jnp.int32, (2 * rows, HEAD_DIM), 0), rows), props
    )
    nothing = jnp.zeros((2 * rows, HEAD_DIM), f32)
    left, values = [], []
    for h in range(head_local):
        part = slice(h * HEAD_DIM, (h + 1) * HEAD_DIM)
        left.append(coeffs[:, part].T.astype(bf16))
        values.append(jnp.concatenate([prev_v[:, part]] * 2, axis=0))

    def take(s, carry):
        own = seq_row == s
        for h in range(head_local):
            right = jnp.concatenate(
                [
                    jnp.concatenate([jnp.where(own, values[h], 0.0), nothing], axis=1),
                    jnp.concatenate([nothing, jnp.where(own, 1.0, 0.0)], axis=1),
                ],
                axis=0,
            ).astype(bf16)
            both = jnp.dot(left[h], right, preferred_element_type=f32)
            fresh = both[:, HEAD_DIM:] * state[s, h] + both[:, :HEAD_DIM]
            taken[s, h] = fresh
            state16[h, :, pl.ds(pl.multiple_of(s * HEAD_DIM, HEAD_DIM), HEAD_DIM)] = fresh.astype(
                bf16
            )
        return carry

    lax.fori_loop(0, seqs, take, 0)
    for copy in locals_[6:]:
        copy.wait()

    def project(source, block, first):
        x = block.astype(f32).reshape(rows, cols)
        lanes = pl.ds(pl.multiple_of(source * cols, cols), cols)
        scaled = (x * gain_v[:, lanes]).astype(bf16)
        term = jnp.dot(scaled, w_all[lanes, :], preferred_element_type=f32)
        if first:
            acc[...] = term
        else:
            acc[...] += term
        return jnp.sum(x * x, axis=1, keepdims=True)

    squares = project(kv, hid[pl.ds(kv * seqs, seqs)], True)
    fwd_copies = {}
    for place, step in enumerate(order):
        source = lax.rem(kv + n_kv - step, n_kv)
        in_copies[step].wait_recv()
        fwd_copies[step] = remote(
            arrived.at[source, mine],
            arrived.at[source, mine],
            fwd_send.at[step],
            fwd_recv.at[step],
            {"tp": peer},
        )
        fwd_copies[step].start()
        if place:
            step = order[place - 1]
            source = lax.rem(kv + n_kv - step, n_kv)
            fwd_copies[step].wait_recv()
            squares += project(source, arrived[source], False)
    step = order[-1]
    source = lax.rem(kv + n_kv - step, n_kv)
    fwd_copies[step].wait_recv()
    squares += project(source, arrived[source], False)

    scale = lax.rsqrt(squares / depth + 1e-06)
    pre = [
        (acc[:, place * width : (place + 1) * width] * scale).astype(bf16).astype(f32)
        for place in range(4)
    ]
    query = jax.nn.silu(pre[0])
    forget = low + (1.0 - low) * jax.nn.sigmoid(pre[1])
    key = 1.0 - forget
    value = pre[2]
    gate = jax.nn.silu(pre[3])
    shifted = [forget] + [pltpu.roll(forget, lag, axis=0) for lag in range(1, props)]
    reach = forget
    for lag in range(1, props):
        reach = reach * jnp.where(at >= lag, shifted[lag], 1.0)
    from_state = (query * reach).astype(bf16)
    near = []
    walk = query
    for lag in range(props):
        if lag:
            walk = walk * shifted[lag - 1]
            near.append(
                (
                    jnp.where(at >= lag, walk * pltpu.roll(key, lag, axis=0), 0.0),
                    pltpu.roll(value, lag, axis=0),
                )
            )
        else:
            near.append((walk * key, value))
    seq_head = lax.div(lax.broadcasted_iota(jnp.int32, (rows, HEAD_DIM), 0), props)
    for h in range(head_local):
        part = slice(h * HEAD_DIM, (h + 1) * HEAD_DIM)
        every = jnp.dot(from_state[:, part], state16[h], preferred_element_type=f32)
        o = jnp.zeros((rows, HEAD_DIM), f32)
        for s in range(seqs):
            o = jnp.where(seq_head == s, every[:, s * HEAD_DIM : (s + 1) * HEAD_DIM], o)
        for weight, fresh in near:
            o += jnp.sum(weight[:, part], axis=1, keepdims=True) * fresh[:, part]
        size = lax.rsqrt(jnp.mean(o * o, axis=1, keepdims=True) + 1e-05)
        heads_all[tp, :, part] = (o * size * head_gain_v[...] * gate[:, part]).astype(bf16)

    tp_copies = {}
    for step in sorted(range(1, n_tp), key=lambda step: -step % 2):
        to = lax.rem(tp + step, n_tp)
        tp_copies[step] = remote(
            heads_all.at[tp], heads_all.at[tp], tp_send.at[step], tp_recv.at[step], {"tp": to}
        )
        tp_copies[step].start()
    for copy in w_o_copies:
        copy.wait()

    def mix(owner):
        lines = pl.ds(pl.multiple_of(owner * width, width), width)
        return jnp.dot(heads_all[owner], w_o[lines, :], preferred_element_type=f32)

    acc_out = mix(tp)
    for step, copy in tp_copies.items():
        copy.wait_recv()
        acc_out += mix(lax.rem(tp + n_tp - step, n_tp))
    for k in range(n_kv):
        blocks[k] = acc_out[:, k * half_cols : (k + 1) * half_cols].astype(bf16)

    out_copies = {}
    for step in order:
        to = lax.rem(kv + step, n_kv)
        out_copies[step] = remote(
            blocks.at[to], landed.at[kv, core], out_send.at[step], out_recv.at[step], {"kv": to}
        )
        out_copies[step].start()
    ofwd = {
        0: remote(
            blocks.at[kv], landed.at[kv, core], ofwd_send.at[0], ofwd_recv.at[0], {"tp": peer}
        )
    }
    ofwd[0].start()
    landed[kv, core] = blocks[kv]
    for step in order:
        source = lax.rem(kv + n_kv - step, n_kv)
        out_copies[step].wait_recv()
        ofwd[step] = remote(
            landed.at[source, core],
            landed.at[source, core],
            ofwd_send.at[step],
            ofwd_recv.at[step],
            {"tp": peer},
        )
        ofwd[step].start()
    for copy in ofwd.values():
        copy.wait_recv()
    for k in range(n_kv):
        out[k * rows : (k + 1) * rows, :] = jnp.concatenate([landed[k, 0], landed[k, 1]], axis=1)
    for group in (in_copies, fwd_copies, tp_copies, out_copies, ofwd):
        for copy in group.values():
            copy.wait_send()


def write_kernel(flat, taken, out, stored, sem):
    pieces = sem.shape[0]
    part = taken.shape[0] // pieces
    copies = []
    for piece in range(pieces):
        some = pl.ds(piece * part, part)
        copies.append(pltpu.make_async_copy(taken.at[some], stored.at[some], sem.at[piece]))
        copies[-1].start()
    out[...] = flat[...].astype(jnp.float32).reshape(out.shape).astype(out.dtype)
    for copy in copies:
        copy.wait()


def fused(
    n_kv,
    n_tp,
    hidden,
    norm_gain,
    w_query,
    w_forget,
    w_input,
    w_outgate,
    w_out,
    floor,
    head_gain,
    base_state,
    prev_forget,
    prev_input,
    accepted,
):
    f32, bf16 = jnp.float32, jnp.bfloat16
    all_seqs, props, cols = hidden.shape
    seqs = all_seqs // n_kv
    rows = seqs * props
    width = w_query.shape[1]
    depth = n_kv * cols
    head_local = width // HEAD_DIM
    anywhere = pl.BlockSpec(memory_space=pl.ANY)
    dma = pltpu.SemaphoreType.DMA
    room = 67043328 - base_state.size * 4 - hidden.size * 2 - 64 * 1024
    out, taken = pl.pallas_call(
        functools.partial(fused_kernel, n_kv, n_tp),
        out_shape=(
            pltpu.VMEM((all_seqs * props, cols), bf16),
            pltpu.VMEM(base_state.shape, f32),
        ),
        in_specs=[anywhere] * 13,
        out_specs=(pl.BlockSpec(memory_space=pltpu.VMEM),) * 2,
        scratch_shapes=[
            pltpu.VMEM(hidden.shape, bf16),
            pltpu.VMEM((n_kv, seqs, props, cols), bf16),
            pltpu.VMEM((1, depth), f32),
            pltpu.VMEM((depth, 4 * width), bf16),
            pltpu.VMEM((n_tp * width, depth // 2), bf16),
            pltpu.VMEM((1, width), f32),
            pltpu.VMEM((1, HEAD_DIM), f32),
            pltpu.VMEM(base_state.shape, f32),
            pltpu.VMEM((head_local, HEAD_DIM, seqs * HEAD_DIM), bf16),
            pltpu.VMEM(prev_forget.shape, bf16),
            pltpu.VMEM(prev_input.shape, bf16),
            pltpu.SMEM(accepted.shape, jnp.int32),
            pltpu.VMEM((rows, 4 * width), f32),
            pltpu.VMEM((n_tp, rows, width), bf16),
            pltpu.VMEM((n_kv, rows, cols // 2), bf16),
            pltpu.VMEM((n_kv, 2, rows, cols // 2), bf16),
            dma((12,)),
            dma((n_kv,)),
            dma((n_kv,)),
            dma((n_kv,)),
            dma((n_kv,)),
            dma((n_kv,)),
            dma((n_tp,)),
            dma((n_tp,)),
            dma((n_kv,)),
            dma((n_kv,)),
            dma((n_kv,)),
            dma((n_kv,)),
        ],
        compiler_params=pltpu.CompilerParams(
            collective_id=0, has_side_effects=True, vmem_limit_bytes=room
        ),
    )(
        accepted,
        hidden,
        norm_gain.reshape(1, depth),
        w_query,
        w_forget,
        w_input,
        w_outgate,
        w_out,
        floor.reshape(1, width),
        head_gain.reshape(1, HEAD_DIM),
        base_state,
        prev_forget,
        prev_input,
    )
    return pl.pallas_call(
        write_kernel,
        out_shape=(
            jax.ShapeDtypeStruct(hidden.shape, bf16),
            jax.ShapeDtypeStruct(base_state.shape, f32),
        ),
        in_specs=[pl.BlockSpec(memory_space=pltpu.VMEM)] * 2,
        out_specs=(pl.BlockSpec(memory_space=pltpu.VMEM), anywhere),
        scratch_shapes=[dma((4 if seqs % 4 == 0 else 1,))],
        compiler_params=pltpu.CompilerParams(vmem_limit_bytes=16 * 1024 * 1024),
    )(out, taken)


def by_shape(n_kv, n_tp, hidden, *rest):
    if hidden.shape[2] % 256 == 0 and n_tp % 2 == 0:
        return fused(n_kv, n_tp, hidden, *rest)
    return shards(hidden, *rest)


def solution(mesh):
    placed = (
        P(None, None, "kv"),
        P(),
        P(None, "tp"),
        P(None, "tp"),
        P(None, "tp"),
        P(None, "tp"),
        P(),
        P("tp"),
        P(),
        P("kv", "tp", None, None),
        P("kv", None, "tp"),
        P("kv", None, "tp"),
        P("kv"),
    )
    return jax.shard_map(
        functools.partial(by_shape, mesh.shape["kv"], mesh.shape["tp"]),
        mesh=mesh,
        in_specs=placed,
        out_specs=(P(None, None, "kv"), P("kv", "tp", None, None)),
        check_vma=False,
    )
```
